32 devices in a mesh: sp: 16 (over z, y, x), tp: 2 (over core).
Axes of the slice: x: 2, y: 2, z: 4, core: 2. Of those that a mesh axis runs over, the one named last changes fastest.
Arguments:
- residual: bfloat16 [4096, 2048], P(('sp', 'tp')), may hold values from -6 to 6
- query_rows: bfloat16 [4096, 1024], P('sp', 'tp'), may hold values from -141 to 141
- key_rows: bfloat16 [4096, 1024], P('sp', 'tp'), may hold values from -7.8 to 7.8
- value_rows: bfloat16 [4096, 1024], P('sp', 'tp'), may hold values from -6 to 6
- mix_lambda: float32 [8], P('tp'), may hold values from 0.3 to 0.8
- documents: int32 [4096], P('sp'), may hold values from 0 to 7, never falling along the last dimension, each value on 1 to 768 neighbouring positions
- out_weight: bfloat16 [1024, 2048], replicated, may hold values from -0.1875 to 0.1875
- norm_gain: float32 [2048], replicated, may hold values from 0.1 to 1.9
- gate_weight: bfloat16 [16, 2048, 2048], P('sp', None, 'tp'), may hold values from -0.125 to 0.125
- up_weight: bfloat16 [16, 2048, 2048], P('sp', None, 'tp'), may hold values from -0.125 to 0.125
- down_weight: bfloat16 [16, 2048, 2048], P('sp', 'tp'), may hold values from -0.125 to 0.125
- routes: int32 [4096, 2], P(('sp', 'tp')), may hold values from 0 to 15, all different within a row; in each aligned block of 128 rows (0 to 127, 128 to 255, ...) at most 32 rows name the same one
- route_weights: float32 [4096, 2], P(('sp', 'tp')), may hold values from 0.25 to 1
Outputs:
- layer_out: bfloat16 [4096, 2048], P(('sp', 'tp'))
The draws below stay inside these ranges and needn't reach their ends.
Inputs may be any that keep to these rules, and one draw needn't show every extreme that they name: `documents`: document numbers never fall along the sequence; a document covers at most 768 positions, and one covers exactly that many. `routes`: each row names two different experts. Among the rows of one index of sp+tp, no expert is named by more than 32 rows, and in every draw some expert is named by exactly 32 rows of some such block.
All inputs are finite; a program needn't handle non-finite values.
Results may differ from the reference program's by a relative error of at most 0.013.
Values may be sent and summed in bfloat16 or wider, within the bound.
A program may use at most 128 MiB of HBM per device.

```python
import math
import jax
import jax.numpy as jnp
import numpy as np
from jax import lax

D = 2048
HEADS = 8
HD = 64
VD = 128
FFE = 2048
TOK_DEV = 256
REACH = 3
TOKENS = 4096
EXPERTS = 16
CAP = 32
DOCS = 8
N_SP = 16
N_TP = 2


def drawn_pair(key):
    shape_rows = (TOKENS, HEADS * 2 * HD)
    base_query = jnp.clip(1.3 * jax.random.normal(jax.random.fold_in(key, 101), shape_rows, jnp.float32), -7.8, 7.8)
    base_keys = jnp.clip(1.3 * jax.random.normal(jax.random.fold_in(key, 102), shape_rows, jnp.float32), -7.8, 7.8)
    return (base_query, base_keys)


def draw_query_rows(key, part):
    return drawn_pair(key)[0].astype(jnp.bfloat16)


def draw_key_rows(key, part):
    return drawn_pair(key)[1].astype(jnp.bfloat16)


def steps_of(rng, dims, pieces, low, high):
    factor_of, own = 1.0, jax.random.fold_in(rng, 6)
    for axis_at, parts in pieces:
        steps = jnp.exp(jax.random.uniform(jax.random.fold_in(own, axis_at), (parts,), jnp.float32, low / len(pieces), high / len(pieces)))
        factor_of = factor_of * jnp.repeat(steps, dims[axis_at] // parts).reshape([-1 if axis == axis_at else 1 for axis in range(len(dims))])
    return factor_of


def split_up(count, total, most, slope):
    loads = [(1 << 20) // math.isqrt(rank ** slope) + 1 for rank in range(2, count + 1)]
    rest, counts = total - most - (count - 1), [1] * (count - 1)
    while rest > 0:
        candidates = [i for i in range(count - 1) if counts[i] < most]
        pool, remaining = sum([loads[i] for i in candidates]), rest
        for i in candidates:
            addition = min(most - counts[i], max(1, remaining * loads[i] // pool), rest)
            counts[i] = counts[i] + addition
            rest = rest - addition
    return np.array([most] + counts)


def uneven_parts(rng, amount, total, limit, lean):
    if amount == 2:
        one = jax.random.randint(rng, (), max(1, total - limit), min(limit, total - 1) + 1)
        return jnp.stack([one, total - one])
    lengths = jnp.asarray(split_up(amount, total, limit, lean), jnp.int32)
    pairs = (amount - 1) // 2
    donor, receiver = lengths[1:1 + 2 * pairs:2], lengths[2:2 + 2 * pairs:2]
    slack = jnp.minimum(donor - 1, limit - receiver)
    shifted = jax.random.randint(jax.random.fold_in(rng, 1), (pairs,), 0, 1 << 20) % (slack + 1)
    lengths = lengths.at[1:1 + 2 * pairs:2].set(donor - shifted).at[2:2 + 2 * pairs:2].set(receiver + shifted)
    return lengths[jax.random.permutation(jax.random.fold_in(rng, 2), amount)]


def assign_block(own_key, own, number, rows, count, top, reach, lean):
    ranking = jax.random.permutation(own_key, count)
    crowded, usual = portions_of(count, rows * top, reach, lean, True), portions_of(count, rows * top, reach, lean, False)
    places = jnp.arange(count)

    def named(sizes, offset_by):
        used = int((sizes > 0).sum())
        fixed = max(1, used // 4)
        passed = fixed + (places - fixed + offset_by * (used - fixed)) % max(1, count - fixed)
        return jnp.zeros((count,), jnp.int32).at[ranking[jnp.where(places < fixed, places, passed)]].set(jnp.asarray(sizes, jnp.int32))

    sizes = jnp.where(number % 4 == 0, named(crowded, number // 4), named(usual, number - number // 4 - 1))
    mixed = jax.random.permutation(jax.random.fold_in(own, 3), count)
    donor, sink = mixed[0:count // 2 * 2:2], mixed[1:count // 2 * 2:2]
    slack = jnp.minimum(sizes[donor] - 1, reach - sizes[sink]) // 2
    slack = jnp.where((donor == ranking[0]) | (sink == ranking[0]) | (sizes[sink] == 0), 0, jnp.maximum(slack, 0))
    passed = jax.random.randint(jax.random.fold_in(own, 4), (count // 2,), 0, 1 << 20) % (slack + 1)
    sizes = sizes.at[donor].add(-passed).at[sink].add(passed)
    items = jnp.searchsorted(jnp.cumsum(sizes), jnp.arange(rows * top), side="right").astype(jnp.int32)
    table = items.reshape(top, rows).T
    table = table[jax.random.permutation(jax.random.fold_in(own, 1), rows)]
    offset_by = jax.random.randint(jax.random.fold_in(own, 2), (rows, 1), 0, top)
    return jnp.take_along_axis(table, (jnp.arange(top)[None, :] + offset_by) % top, axis=1)


def portions_of(amount, total, reach, slope, full):
    weights = [(1 << 20) // math.isqrt(grade ** slope) + 1 for grade in range(1, amount + 1)]
    largest = reach if full else min(reach, max(-(-total // amount), total * weights[0] // sum(weights)))
    least = 1 if total - largest >= amount - 1 else 0
    holding, rest = [largest] + [least] * (amount - 1), total - largest - least * (amount - 1)
    while rest > 0:
        candidates = [i for i in range(1, amount) if holding[i] < largest] or [i for i in range(1, amount) if holding[i] < reach]
        pool, budget = sum([weights[i] for i in candidates]), rest
        for i in candidates:
            more = min(reach - holding[i], max(1, budget * weights[i] // pool), rest)
            holding[i] = holding[i] + more
            rest = rest - more
    return np.array(holding)


def normal_values(own_key, shape, deviation, limit, cuts=(), held_as=jnp.bfloat16):
    level = steps_of(own_key, shape, cuts, -0.22, 0.18) if cuts else 1.0
    values = jax.random.normal(own_key, shape, jnp.float32) * deviation * level
    return jnp.minimum(jnp.maximum(values, -limit), limit).astype(held_as)


def setup_inputs(seed: int = 0) -> dict:
    keys = jax.random.split(jax.random.key(seed), 14)
    residual = normal_values(keys[0], (TOKENS, D), 1.0, 6.0, ((0, 32),))
    query_rows = draw_query_rows(jax.random.fold_in(keys[13], 71), 0)
    key_rows = draw_key_rows(jax.random.fold_in(keys[13], 71), 0)
    value_rows = normal_values(keys[3], (TOKENS, HEADS * VD), 1.0, 6.0, ((0, 16), (1, 2)))
    mix_lambda = jnp.clip(0.3 + 0.5 * jax.random.uniform(keys[4], (HEADS,), jnp.float32) ** steps_of(keys[4], (HEADS,), ((0, 2),), -0.2, 0.2), 0.3, 0.8)
    documents = jnp.searchsorted(jnp.cumsum(uneven_parts(keys[5], DOCS, TOKENS, REACH * TOK_DEV, 0)), jnp.arange(TOKENS), side="right").astype(jnp.int32)
    out_weight = normal_values(keys[6], (HEADS * VD, D), (HEADS * VD) ** -0.5, 0.1875)
    norm_gain = jnp.clip(1.0 + 0.18 * jax.random.normal(keys[7], (D,), jnp.float32), 0.1, 1.9)
    gate_weight = normal_values(keys[8], (EXPERTS, D, FFE), D ** -0.5, 0.125, ((0, 16), (2, 2)))
    up_weight = normal_values(keys[9], (EXPERTS, D, FFE), D ** -0.5, 0.125, ((0, 16), (2, 2)))
    down_weight = normal_values(keys[10], (EXPERTS, FFE, D), FFE ** -0.5, 0.125, ((0, 16), (1, 2)))
    routes_keys = jax.random.split(jax.random.fold_in(keys[11], 1), TOKENS // (TOK_DEV // 2))
    routes_turns = jax.random.permutation(jax.random.fold_in(keys[11], 3), TOKENS // (TOK_DEV // 2))
    routes = jax.vmap(lambda own, number: assign_block(jax.random.fold_in(keys[11], 2), own, number, TOK_DEV // 2, EXPERTS, 2, CAP, 2))(routes_keys, routes_turns).reshape((TOKENS, 2))
    route_weights = jnp.clip(0.25 + 0.75 * jax.random.uniform(keys[12], (TOKENS, 2), jnp.float32) ** steps_of(keys[12], (TOKENS, 2), ((0, 32),), -0.2, 0.2), 0.25, 1.0)
    return {"residual": residual, "query_rows": query_rows, "key_rows": key_rows, "value_rows": value_rows, "mix_lambda": mix_lambda, "documents": documents, "out_weight": out_weight, "norm_gain": norm_gain, "gate_weight": gate_weight, "up_weight": up_weight, "down_weight": down_weight, "routes": routes, "route_weights": route_weights}


def rms_rows(values_in):
    return values_in * lax.rsqrt(lax.optimization_barrier(jnp.mean(values_in * values_in, axis=-1, keepdims=True)) + 1e-06)

def reference(residual, query_rows, key_rows, value_rows, mix_lambda, documents, out_weight, norm_gain, gate_weight, up_weight, down_weight, routes, route_weights):
    score_scale = HD ** (-0.5)
    queries = query_rows.reshape(TOKENS // TOK_DEV, TOK_DEV, HEADS, 2, HD)
    all_keys = key_rows.reshape(TOKENS, HEADS, 2, HD).astype(jnp.float32)
    all_values = value_rows.reshape(TOKENS, HEADS, VD).astype(jnp.float32)
    block_ids = documents.reshape(TOKENS // TOK_DEV, TOK_DEV)

    def attend(operands):
        block_query, query_ids = operands
        scores = jnp.einsum('qhcd,khcd->hcqk', block_query.astype(jnp.float32), all_keys) * score_scale
        same_document = query_ids[:, None] == documents[None, :]
        masked = jnp.where(same_document[None, None], scores, -1e+30)
        largest = lax.optimization_barrier(jnp.max(masked, axis=-1, keepdims=True))
        lifted = jnp.exp(masked - largest)
        probabilities = lifted / lax.optimization_barrier(jnp.sum(lifted, axis=-1, keepdims=True))
        weights = (probabilities[:, 0] - mix_lambda[:, None, None] * probabilities[:, 1]).astype(jnp.bfloat16)
        head_out = jnp.einsum('hqk,khd->qhd', weights.astype(jnp.float32), all_values)
        head_normed = rms_rows(head_out).astype(jnp.bfloat16)
        return head_normed.reshape(TOK_DEV, HEADS * VD)
    head_rows = lax.map(attend, (queries, block_ids)).reshape(TOKENS, HEADS * VD)
    projected = jnp.dot(head_rows, out_weight, preferred_element_type=jnp.float32)
    mixed = (residual.astype(jnp.float32) + projected).astype(jnp.bfloat16)
    normed = (rms_rows(mixed.astype(jnp.float32)) * norm_gain).astype(jnp.bfloat16)
    top_count = routes.shape[1]
    assign_count = TOKENS * top_count
    flat_routes = routes.reshape(-1)
    padded_rows = jnp.concatenate([normed, jnp.zeros((1, D), jnp.bfloat16)], axis=0)
    most_rows = N_SP * N_TP * CAP
    half_width = FFE // N_TP

    def one_expert(collected, expert):
        chosen = jnp.nonzero(flat_routes == expert, size=most_rows, fill_value=assign_count)[0].astype(jnp.int32)
        picked = padded_rows[chosen // top_count]
        gate = jnp.dot(picked, gate_weight[expert], preferred_element_type=jnp.float32)
        upward = jnp.dot(picked, up_weight[expert], preferred_element_type=jnp.float32)
        hidden = (jax.nn.silu(gate) * upward).astype(jnp.bfloat16)
        hidden_halves = hidden.reshape(most_rows, N_TP, half_width).astype(jnp.float32)
        down_halves = down_weight[expert].reshape(N_TP, half_width, D).astype(jnp.float32)
        partial_value = jnp.einsum('rhp,hpd->hrd', hidden_halves, down_halves).astype(jnp.bfloat16)
        expert_out = lax.optimization_barrier(jnp.sum(partial_value.astype(jnp.float32), axis=0)).astype(jnp.bfloat16)
        return (collected.at[chosen].set(expert_out), None)
    collected, _ = lax.scan(one_expert, jnp.zeros((assign_count + 1, D), jnp.bfloat16), jnp.arange(EXPERTS, dtype=jnp.int32))
    outputs = collected[:assign_count].reshape(TOKENS, top_count, D).astype(jnp.float32)
    weighted = lax.optimization_barrier(jnp.sum(outputs * route_weights[:, :, None], axis=1))
    return (mixed.astype(jnp.float32) + weighted).astype(jnp.bfloat16)
```

```python
import functools

import jax
import jax.numpy as jnp
from jax import lax
from jax.experimental import pallas as pl
from jax.experimental.pallas import tpu as pltpu
from jax.sharding import PartitionSpec as P

HD = 64
REACH = 3
MESH = pl.DeviceIdType.MESH
VMEM = pl.BlockSpec(memory_space=pltpu.VMEM)


def attend_kernel(
    groups,
    lambda_ref,
    q_ref,
    k_ref,
    v_ref,
    id_ref,
    residual_ref,
    gain_ref,
    proj_hbm,
    mixed_ref,
    normed_ref,
    q_all,
    k_all,
    v_all,
    id_all,
    out_buf,
    heads_ref,
    proj_ref,
    square_ref,
    proj_sem,
    in_send,
    in_recv,
    hop_send,
    hop_recv,
    out_send,
    out_recv,
):
    me, core = lax.axis_index("sp"), lax.axis_index("tp")
    per = REACH + 1
    g, p = me // per, me % per
    length, wide = q_all.shape[1:]
    value_dim = v_all.shape[2]
    rows = mixed_ref.shape[0]
    cores = length // rows
    span = 2 * REACH + 1
    barrier = pltpu.get_barrier_semaphore()

    for side in range(cores):
        for j in range(per):

            @pl.when(jnp.logical_or(side != core, j > 0))
            def _():
                at = g * per + (p + j) % per
                pl.semaphore_signal(barrier, inc=1, device_id=(at, side), device_id_type=MESH)

    def beyond(step):
        return jnp.logical_and(g + step >= 0, g + step < groups)

    for step in (1, -1):

        @pl.when(beyond(step))
        def _():
            at = me + step * per
            pl.semaphore_signal(barrier, inc=1, device_id=(at, core), device_id_type=MESH)

    others = cores * per - 1
    pl.semaphore_wait(barrier, others + jnp.minimum(g, 1) + jnp.minimum(groups - 1 - g, 1))

    def remote(source, target, sent, came, at, side):
        return pltpu.make_async_remote_copy(
            src_ref=source,
            dst_ref=target,
            send_sem=sent,
            recv_sem=came,
            device_id=(at, side),
            device_id_type=MESH,
        )

    def head_cut(head, width):
        return pl.ds(pl.multiple_of(head * width, width), width)

    def id_cut(slot):
        return pl.ds(pl.multiple_of(slot * length, length), length)

    def own_part(which, head):
        return (
            id_ref,
            k_ref.at[:, head_cut(head, wide)],
            v_ref.at[:, head_cut(head, value_dim)],
            q_ref.at[:, head_cut(head, wide)],
        )[which]

    def place_of(which, slot):
        return (
            id_all.at[:, id_cut(slot)],
            k_all.at[slot],
            v_all.at[slot],
            q_all.at[slot - REACH],
        )[which]

    def scatter(j, which):
        to = (p + j) % per
        return remote(
            own_part(which, to),
            place_of(which, REACH + p),
            in_send.at[j - 1, which],
            in_recv.at[j - 1, which],
            g * per + to,
            core,
        )

    def scattered(j, which):
        source = (p + per - j) % per
        return remote(
            own_part(which, source),
            place_of(which, REACH + source),
            in_send.at[j - 1, which],
            in_recv.at[j - 1, which],
            g * per + source,
            core,
        )

    def hop(step, q, which, own):
        at = 0 if step > 0 else 1
        source = own_part(which, p) if own else place_of(which, REACH + q)
        return remote(
            source,
            place_of(which, REACH + q - step * per),
            hop_send.at[at, q, which],
            hop_recv.at[at, q, which],
            me + step * per,
            core,
        )

    def hopped(step, q, which):
        at = 0 if step > 0 else 1
        return remote(
            own_part(which, p),
            place_of(which, REACH + q - step * per),
            hop_send.at[at, q, which],
            hop_recv.at[at, q, which],
            me - step * per,
            core,
        )

    def hops(step, q):
        return jnp.logical_and(beyond(step), q > 0 if step > 0 else q < REACH)

    for which in range(4):
        for j in range(1, per):
            scatter(j, which).start()
        if which < 3:
            for step in (1, -1):

                @pl.when(hops(step, p))
                def _():
                    hop(step, p, which, True).start()

    load = pltpu.make_async_copy(proj_hbm, proj_ref, proj_sem)
    load.start()
    k_all[REACH + p] = k_ref[:, head_cut(p, wide)]
    v_all[REACH + p] = v_ref[:, head_cut(p, value_dim)]
    q_all[p] = q_ref[:, head_cut(p, wide)]
    id_all[:, id_cut(REACH + p)] = id_ref[...]
    for step in (1, -1):

        @pl.when(jnp.logical_not(beyond(-step)))
        def _():
            for slot in range(REACH):
                at = slot if step > 0 else span + slot
                k_all[at] = jnp.zeros_like(k_all[at])
                v_all[at] = jnp.zeros_like(v_all[at])
                id_all[:, at * length : (at + 1) * length] = jnp.full(
                    (1, length), -1, id_all.dtype
                )

    for which in range(3):
        for j in range(1, per):
            scattered(j, which).wait_recv()
            q = (p + per - j) % per
            for step in (1, -1):

                @pl.when(hops(step, q))
                def _():
                    hop(step, q, which, False).start()

    for j in range(1, per):
        scattered(j, 3).wait_recv()
    for which in range(3):
        for q in range(per):
            for step in (1, -1):
                if 0 <= REACH + q - step * per < span + REACH:

                    @pl.when(beyond(-step))
                    def _():
                        hopped(step, q, which).wait_recv()

    scale = jnp.asarray(HD ** (-0.5), q_all.dtype)
    contract = (((1,), (1,)), ((), ()))
    head = core * per + p

    def give(it):
        i, half = (p + 1 + it // cores) % per, (core + 1 + it) % cores
        return remote(
            out_buf.at[it],
            heads_ref.at[:, head_cut(head, value_dim)],
            out_send.at[it],
            out_recv.at[head],
            g * per + i,
            half,
        )

    def taken(source):
        return remote(
            out_buf.at[0],
            heads_ref.at[:, head_cut(source, value_dim)],
            out_send.at[0],
            out_recv.at[source],
            g * per + source % per,
            source // per,
        )

    @pl.loop(0, cores * per)
    def _(it):
        i, half = (p + 1 + it // cores) % per, (core + 1 + it) % cores
        first_row = pl.multiple_of(half * rows, rows)
        query = q_all[i, pl.ds(first_row, rows), :]
        lane = lax.broadcasted_iota(jnp.int32, query.shape, 1)
        own = id_all[:, pl.ds(pl.multiple_of((REACH + i) * length + half * rows, rows), rows)]
        own = jnp.transpose(jnp.broadcast_to(own, (128, rows)))[:, :1]
        ids = id_all[:, pl.ds(pl.multiple_of(i * length, length), span * length)]
        same = own == ids
        keys = k_all[pl.ds(i, span)].reshape(span * length, wide)
        values = v_all[pl.ds(i, span)].reshape(span * length, value_dim)

        def lifted(keep):
            part = jnp.where(keep, query * scale, jnp.zeros_like(query))
            scores = lax.dot_general(part, keys, contract, preferred_element_type=jnp.float32)
            masked = jnp.where(same, scores, -1e30)
            powers = jnp.exp(masked - jnp.max(masked, axis=-1, keepdims=True))
            return powers, jnp.sum(powers, axis=-1, keepdims=True)

        first, first_sum = lifted(lane < HD)
        second, second_sum = lifted(lane >= HD)
        weights = first * (1.0 / first_sum) - second * (lambda_ref[p] / second_sum)
        head_out = jnp.dot(
            weights.astype(jnp.bfloat16), values, preferred_element_type=jnp.float32
        )
        scaled = head_out * lax.rsqrt(
            jnp.mean(head_out * head_out, axis=-1, keepdims=True) + 1e-06
        )
        out_buf[it] = scaled.astype(jnp.bfloat16)

        @pl.when(it > 0)
        def _():
            give(it - 1).start()

    last = cores * per - 1
    heads_ref[:, head_cut(head, value_dim)] = out_buf[last]
    load.wait()
    for source in range(cores * per):

        @pl.when(source != head)
        def _():
            taken(source).wait_recv()

    model = mixed_ref.shape[1]
    chunk = min(256, model)
    square_ref[...] = jnp.zeros_like(square_ref)

    @pl.loop(0, model // chunk)
    def _(c):
        cut = head_cut(c, chunk)
        projected = jnp.dot(heads_ref[...], proj_ref[:, cut], preferred_element_type=jnp.float32)
        mixed = (residual_ref[:, cut].astype(jnp.float32) + projected).astype(jnp.bfloat16)
        mixed_ref[:, cut] = mixed
        mixed_wide = mixed.astype(jnp.float32)
        square_ref[...] += jnp.sum(mixed_wide * mixed_wide, axis=-1, keepdims=True)

    factor = lax.rsqrt(square_ref[...] * (1.0 / model) + 1e-06)

    @pl.loop(0, model // chunk)
    def _(c):
        cut = head_cut(c, chunk)
        mixed_wide = mixed_ref[:, cut].astype(jnp.float32)
        normed_ref[:, cut] = (mixed_wide * factor * gain_ref[:, cut]).astype(jnp.bfloat16)

    for which in range(4):
        for j in range(1, per):
            scatter(j, which).wait_send()
    for which in range(3):
        for q in range(per):
            for step in (1, -1):

                @pl.when(hops(step, q))
                def _():
                    hop(step, q, which, False).wait_send()

    for it in range(last):
        give(it).wait_send()


def attend(count, query_rows, key_rows, value_rows, ids, mix_lambda, residual, gain, out_weight):
    length, width = query_rows.shape
    per = REACH + 1
    wide, value_dim = width // per, value_rows.shape[1] // per
    rows, model = residual.shape
    blocks = 3 * REACH + 1
    outs = length // rows * per
    kept = jnp.bfloat16
    shape = jax.ShapeDtypeStruct((rows, model), kept)
    dma = pltpu.SemaphoreType.DMA
    smem = pl.BlockSpec(memory_space=pltpu.SMEM)
    anywhere = pl.BlockSpec(memory_space=pl.ANY)
    return pl.pallas_call(
        functools.partial(attend_kernel, count // per),
        out_shape=[shape, shape],
        in_specs=[smem] + [VMEM] * 6 + [anywhere],
        out_specs=[VMEM] * 2,
        scratch_shapes=[
            pltpu.VMEM((per, length, wide), kept),
            pltpu.VMEM((blocks, length, wide), kept),
            pltpu.VMEM((blocks, length, value_dim), kept),
            pltpu.VMEM((1, blocks * length), jnp.int32),
            pltpu.VMEM((outs, rows, value_dim), kept),
            pltpu.VMEM((rows, outs * value_dim), kept),
            pltpu.VMEM(out_weight.shape, kept),
            pltpu.VMEM((rows, 1), jnp.float32),
            dma,
            dma((per - 1, 4)),
            dma((per - 1, 4)),
            dma((2, per, 3)),
            dma((2, per, 3)),
            dma((outs,)),
            dma((outs,)),
        ],
        compiler_params=pltpu.CompilerParams(collective_id=0, has_side_effects=True),
        name="attend",
    )(mix_lambda, query_rows, key_rows, value_rows, ids, residual, gain, out_weight)


def greet_all(count, me, core):
    barrier = pltpu.get_barrier_semaphore()
    pl.semaphore_signal(barrier, inc=1, device_id=(me, 1 - core), device_id_type=MESH)

    @pl.loop(1, count)
    def _(step):
        pl.semaphore_signal(
            barrier, inc=1, device_id=((me + step) % count, core), device_id_type=MESH
        )

    pl.semaphore_wait(barrier, count)


def experts_kernel(
    count,
    out_ref,
    gate_hbm,
    up_hbm,
    down_hbm,
    back_ref,
    rows_ref,
    part_ref,
    far_ref,
    sum_ref,
    hidden_ref,
    gate_ref,
    up_ref,
    down_ref,
    load_sem,
    own_sem,
    send_sem,
    recv_sem,
    pass_sem,
    come_sem,
    swap_sem,
    half_sem,
    give_sem,
    take_sem,
):
    me, core = lax.axis_index("sp"), lax.axis_index("tp")
    per = rows_ref.shape[2]
    groups = count // per
    layer, place = me // per, me % per
    greet_all(count, me, core)

    def ahead(g, j):
        return (layer + g) % groups * per + (place + j) % per

    def behind(g, j):
        return (layer - g + groups) % groups * per + (place - j + per) % per

    def remote(source, target, sent, came, at, side):
        return pltpu.make_async_remote_copy(
            src_ref=source,
            dst_ref=target,
            send_sem=sent,
            recv_sem=came,
            device_id=(at, side),
            device_id_type=MESH,
        )

    def across(g, j):
        at = ahead(g, j)
        return remote(
            out_ref.at[at], rows_ref.at[g, core, j], send_sem.at[g, j], recv_sem.at[g, j], at, core
        )

    def forward(g, j, side):
        block = rows_ref.at[g, side, j]
        return remote(block, block, pass_sem.at[g, j], come_sem.at[g, j], me, 1 - core)

    def swap(g):
        return remote(
            part_ref.at[g, 1 - core], far_ref.at[g], swap_sem.at[g], half_sem.at[g], me, 1 - core
        )

    def home(g, j):
        at = behind(g, j)
        return remote(
            sum_ref.at[g, j], back_ref.at[me], give_sem.at[g, j], take_sem.at[g, j], at, core
        )

    def came_home(g, j):
        at = ahead(g, j)
        return remote(
            sum_ref.at[g, j], back_ref.at[at], give_sem.at[g, j], take_sem.at[g, j], at, core
        )

    own = pltpu.make_async_copy(out_ref.at[me], rows_ref.at[0, core, 0], own_sem)
    own.start()

    @pl.loop(1, count)
    def _(step):
        across(step // per, step % per).start()

    loads = [
        pltpu.make_async_copy(source, target, load_sem.at[which])
        for which, (source, target) in enumerate(
            ((gate_hbm, gate_ref), (up_hbm, up_ref), (down_hbm, down_ref))
        )
    ]
    for load in loads:
        load.start()
    own.wait()
    forward(0, 0, core).start()

    @pl.loop(0, groups)
    def _(g):
        for j in range(per):

            @pl.when(g + j > 0)
            def _():
                across(g, j).wait_recv()
                forward(g, j, core).start()

        for j in range(per):
            forward(g, j, 1 - core).wait_recv()

        @pl.when(g == 0)
        def _():
            for load in loads:
                load.wait()

        rows, width = hidden_ref.shape
        model = down_ref.shape[1]
        wide = min(256, width)

        @pl.loop(0, width // wide)
        def _(c):
            cut = pl.ds(pl.multiple_of(c * wide, wide), wide)
            taken = rows_ref[g].reshape(rows, model)
            gate = jnp.dot(taken, gate_ref[:, cut], preferred_element_type=jnp.float32)
            upward = jnp.dot(taken, up_ref[:, cut], preferred_element_type=jnp.float32)
            hidden_ref[:, cut] = (gate / (1.0 + jnp.exp(-gate)) * upward).astype(hidden_ref.dtype)

        @pl.loop(0, model // wide)
        def _(c):
            cut = pl.ds(pl.multiple_of(c * wide, wide), wide)
            product = jnp.dot(
                hidden_ref[...], down_ref[:, cut], preferred_element_type=jnp.float32
            ).astype(part_ref.dtype)
            part_ref[g, :, :, :, cut] = product.reshape(part_ref.shape[1:4] + (wide,))

        swap(g).start()
        swap(g).wait_recv()
        for j in range(per):
            mine = part_ref[g, core, j].astype(jnp.float32)
            sum_ref[g, j] = (mine + far_ref[g, j].astype(jnp.float32)).astype(sum_ref.dtype)
            if j > 0:

                @pl.when(g + j > 1)
                def _():
                    home(g, j - 1).start()

        home(g, per - 1).start()

    back_ref[me] = sum_ref[0, 0]

    @pl.loop(1, count)
    def _(step):
        g, j = step // per, step % per
        came_home(g, j).wait_recv()
        home(g, j).wait_send()
        across(g, j).wait_send()

    @pl.loop(0, count)
    def _(step):
        forward(step // per, step % per, core).wait_send()

    @pl.loop(0, groups)
    def _(g):
        swap(g).wait_send()


def run_experts(count, outgoing, gate_weight, up_weight, down_weight):
    _, capacity, model = outgoing.shape
    per = REACH + 1
    groups = count // per
    hidden = gate_weight.shape[1]
    kept = outgoing.dtype
    each = pltpu.SemaphoreType.DMA((groups, per))
    whole = pltpu.SemaphoreType.DMA((groups,))
    anywhere = pl.BlockSpec(memory_space=pl.ANY)
    return pl.pallas_call(
        functools.partial(experts_kernel, count),
        out_shape=jax.ShapeDtypeStruct(outgoing.shape, kept),
        in_specs=[VMEM, anywhere, anywhere, anywhere],
        out_specs=VMEM,
        scratch_shapes=[
            pltpu.VMEM((groups, 2, per, capacity, model), kept),
            pltpu.VMEM((groups, 2, per, capacity, model), kept),
            pltpu.VMEM((groups, per, capacity, model), kept),
            pltpu.VMEM((groups, per, capacity, model), kept),
            pltpu.VMEM((2 * per * capacity, hidden), kept),
            pltpu.VMEM(gate_weight.shape, kept),
            pltpu.VMEM(up_weight.shape, kept),
            pltpu.VMEM(down_weight.shape, kept),
            pltpu.SemaphoreType.DMA((3,)),
            pltpu.SemaphoreType.DMA,
            each,
            each,
            each,
            each,
            whole,
            whole,
            each,
            each,
        ],
        compiler_params=pltpu.CompilerParams(collective_id=1, has_side_effects=True),
        name="experts",
    )(outgoing, gate_weight, up_weight, down_weight)


def slots_of(routes, experts, capacity):
    flat_routes = routes.reshape(-1)
    table = (flat_routes[:, None] == jnp.arange(experts, dtype=jnp.int32)[None, :]).astype(
        jnp.float32
    )
    count = table.shape[0]
    before = jnp.tril(jnp.ones((count, count), jnp.bfloat16), -1)
    earlier = jnp.dot(before, table.astype(jnp.bfloat16), preferred_element_type=jnp.float32)
    rank = jnp.sum(earlier * table, axis=1).astype(jnp.int32)
    return (flat_routes * capacity + rank).reshape(routes.shape)


def on_device(
    residual,
    query_rows,
    key_rows,
    value_rows,
    mix_lambda,
    documents,
    out_weight,
    norm_gain,
    gate_weight,
    up_weight,
    down_weight,
    routes,
    route_weights,
):
    length = query_rows.shape[0]
    model_width = residual.shape[1]
    experts = lax.axis_size("sp")
    capacity = 2 * length // experts
    top_count = routes.shape[1]
    mixed, normed = attend(
        experts,
        query_rows,
        key_rows,
        value_rows,
        documents.reshape(1, length),
        mix_lambda,
        residual,
        norm_gain.reshape(1, model_width),
        out_weight,
    )
    mixed_wide = mixed.astype(jnp.float32)
    slots = slots_of(routes, experts, capacity)
    places = jnp.arange(experts * capacity, dtype=jnp.int32)
    spread = jnp.any(slots[None, :, :] == places[:, None, None], axis=-1).astype(jnp.bfloat16)
    outgoing = jnp.dot(spread, normed, preferred_element_type=jnp.float32).astype(jnp.bfloat16)
    returned = run_experts(
        experts,
        outgoing.reshape(experts, capacity, model_width),
        gate_weight[0],
        up_weight[0],
        down_weight[0],
    ).reshape(-1, model_width)
    weighted = 0.0
    for which in range(top_count):
        pick = (slots[:, which][:, None] == places[None, :]).astype(jnp.bfloat16)
        picked = jnp.dot(pick, returned, preferred_element_type=jnp.float32)
        weighted = weighted + picked * route_weights[:, which][:, None]
    return (mixed_wide + weighted).astype(jnp.bfloat16)


def solution(mesh):
    placed = (
        P(("sp", "tp"), None),
        P("sp", "tp"),
        P("sp", "tp"),
        P("sp", "tp"),
        P("tp"),
        P("sp"),
        P(),
        P(),
        P("sp", None, "tp"),
        P("sp", None, "tp"),
        P("sp", "tp", None),
        P(("sp", "tp"), None),
        P(("sp", "tp"), None),
    )
    return jax.shard_map(
        on_device, mesh=mesh, in_specs=placed, out_specs=P(("sp", "tp"), None), check_vma=False
    )
```

```python
import functools

import jax
import jax.numpy as jnp
from jax import lax
from jax.experimental import pallas as pl
from jax.experimental.pallas import tpu as pltpu
from jax.sharding import PartitionSpec as P

HD = 64
REACH = 3
MESH = pl.DeviceIdType.MESH
VMEM = pl.BlockSpec(memory_space=pltpu.VMEM)


def attend_kernel(
    groups,
    lambda_ref,
    q_ref,
    k_ref,
    v_ref,
    id_ref,
    residual_ref,
    gain_ref,
    proj_hbm,
    mixed_ref,
    normed_ref,
    q_all,
    k_all,
    v_all,
    id_all,
    out_buf,
    heads_ref,
    proj_ref,
    square_ref,
    proj_sem,
    in_send,
    in_recv,
    hop_send,
    hop_recv,
    out_send,
    out_recv,
):
    me, core = lax.axis_index("sp"), lax.axis_index("tp")
    per = REACH + 1
    g, p = me // per, me % per
    length, wide = q_all.shape[1:]
    value_dim = v_all.shape[2]
    rows = mixed_ref.shape[0]
    cores = length // rows
    span = 2 * REACH + 1
    barrier = pltpu.get_barrier_semaphore()

    for side in range(cores):
        for j in range(per):

            @pl.when(jnp.logical_or(side != core, j > 0))
            def _():
                at = g * per + (p + j) % per
                pl.semaphore_signal(barrier, inc=1, device_id=(at, side), device_id_type=MESH)

    def beyond(step):
        return jnp.logical_and(g + step >= 0, g + step < groups)

    for step in (1, -1):

        @pl.when(beyond(step))
        def _():
            at = me + step * per
            pl.semaphore_signal(barrier, inc=1, device_id=(at, core), device_id_type=MESH)

    others = cores * per - 1
    pl.semaphore_wait(barrier, others + jnp.minimum(g, 1) + jnp.minimum(groups - 1 - g, 1))

    def remote(source, target, sent, came, at, side):
        return pltpu.make_async_remote_copy(
            src_ref=source,
            dst_ref=target,
            send_sem=sent,
            recv_sem=came,
            device_id=(at, side),
            device_id_type=MESH,
        )

    def head_cut(head, width):
        return pl.ds(pl.multiple_of(head * width, width), width)

    def id_cut(slot):
        return pl.ds(pl.multiple_of(slot * length, length), length)

    def own_part(which, head):
        return (
            id_ref,
            k_ref.at[:, head_cut(head, wide)],
            v_ref.at[:, head_cut(head, value_dim)],
            q_ref.at[:, head_cut(head, wide)],
        )[which]

    def place_of(which, slot):
        return (
            id_all.at[:, id_cut(slot)],
            k_all.at[slot],
            v_all.at[slot],
            q_all.at[slot - REACH],
        )[which]

    def scatter(j, which):
        to = (p + j) % per
        return remote(
            own_part(which, to),
            place_of(which, REACH + p),
            in_send.at[j - 1, which],
            in_recv.at[j - 1, which],
            g * per + to,
            core,
        )

    def scattered(j, which):
        source = (p + per - j) % per
        return remote(
            own_part(which, source),
            place_of(which, REACH + source),
            in_send.at[j - 1, which],
            in_recv.at[j - 1, which],
            g * per + source,
            core,
        )

    def hop(step, q, which, own):
        at = 0 if step > 0 else 1
        source = own_part(which, p) if own else place_of(which, REACH + q)
        return remote(
            source,
            place_of(which, REACH + q - step * per),
            hop_send.at[at, q, which],
            hop_recv.at[at, q, which],
            me + step * per,
            core,
        )

    def hopped(step, q, which):
        at = 0 if step > 0 else 1
        return remote(
            own_part(which, p),
            place_of(which, REACH + q - step * per),
            hop_send.at[at, q, which],
            hop_recv.at[at, q, which],
            me - step * per,
            core,
        )

    def hops(step, q):
        return jnp.logical_and(beyond(step), q > 0 if step > 0 else q < REACH)

    for which in range(4):
        for j in range(1, per):
            scatter(j, which).start()
        if which < 3:
            for step in (1, -1):

                @pl.when(hops(step, p))
                def _():
                    hop(step, p, which, True).start()

    load = pltpu.make_async_copy(proj_hbm, proj_ref, proj_sem)
    load.start()
    k_all[REACH + p] = k_ref[:, head_cut(p, wide)]
    v_all[REACH + p] = v_ref[:, head_cut(p, value_dim)]
    q_all[p] = q_ref[:, head_cut(p, wide)]
    id_all[:, id_cut(REACH + p)] = id_ref[...]
    for step in (1, -1):

        @pl.when(jnp.logical_not(beyond(-step)))
        def _():
            for slot in range(REACH):
                at = slot if step > 0 else span + slot
                k_all[at] = jnp.zeros_like(k_all[at])
                v_all[at] = jnp.zeros_like(v_all[at])
                id_all[:, at * length : (at + 1) * length] = jnp.full(
                    (1, length), -1, id_all.dtype
                )

    for which in range(3):
        for j in range(1, per):
            scattered(j, which).wait_recv()
            q = (p + per - j) % per
            for step in (1, -1):

                @pl.when(hops(step, q))
                def _():
                    hop(step, q, which, False).start()

    for j in range(1, per):
        scattered(j, 3).wait_recv()
    for which in range(3):
        for q in range(per):
            for step in (1, -1):
                if 0 <= REACH + q - step * per < span + REACH:

                    @pl.when(beyond(-step))
                    def _():
                        hopped(step, q, which).wait_recv()

    scale = jnp.asarray(HD ** (-0.5), q_all.dtype)
    contract = (((1,), (1,)), ((), ()))
    head = core * per + p

    def give(it):
        i, half = (p + 1 + it // cores) % per, (core + 1 + it) % cores
        return remote(
            out_buf.at[it],
            heads_ref.at[:, head_cut(head, value_dim)],
            out_send.at[it],
            out_recv.at[head],
            g * per + i,
            half,
        )

    def taken(source):
        return remote(
            out_buf.at[0],
            heads_ref.at[:, head_cut(source, value_dim)],
            out_send.at[0],
            out_recv.at[source],
            g * per + source % per,
            source // per,
        )

    @pl.loop(0, cores * per)
    def _(it):
        i, half = (p + 1 + it // cores) % per, (core + 1 + it) % cores
        first_row = pl.multiple_of(half * rows, rows)
        query = q_all[i, pl.ds(first_row, rows), :]
        lane = lax.broadcasted_iota(jnp.int32, query.shape, 1)
        own = id_all[:, pl.ds(pl.multiple_of((REACH + i) * length + half * rows, rows), rows)]
        own = jnp.transpose(jnp.broadcast_to(own, (128, rows)))[:, :1]
        ids = id_all[:, pl.ds(pl.multiple_of(i * length, length), span * length)]
        same = own == ids
        keys = k_all[pl.ds(i, span)].reshape(span * length, wide)
        values = v_all[pl.ds(i, span)].reshape(span * length, value_dim)

        def lifted(keep):
            part = jnp.where(keep, query * scale, jnp.zeros_like(query))
            scores = lax.dot_general(part, keys, contract, preferred_element_type=jnp.float32)
            masked = jnp.where(same, scores, -1e30)
            powers = jnp.exp(masked - jnp.max(masked, axis=-1, keepdims=True))
            return powers, jnp.sum(powers, axis=-1, keepdims=True)

        first, first_sum = lifted(lane < HD)
        second, second_sum = lifted(lane >= HD)
        weights = first * (1.0 / first_sum) - second * (lambda_ref[p] / second_sum)
        head_out = jnp.dot(
            weights.astype(jnp.bfloat16), values, preferred_element_type=jnp.float32
        )
        scaled = head_out * lax.rsqrt(
            jnp.mean(head_out * head_out, axis=-1, keepdims=True) + 1e-06
        )
        out_buf[it] = scaled.astype(jnp.bfloat16)

        @pl.when(it > 0)
        def _():
            give(it - 1).start()

    last = cores * per - 1
    heads_ref[:, head_cut(head, value_dim)] = out_buf[last]
    load.wait()
    for source in range(cores * per):

        @pl.when(source != head)
        def _():
            taken(source).wait_recv()

    model = mixed_ref.shape[1]
    chunk = min(256, model)
    square_ref[...] = jnp.zeros_like(square_ref)

    @pl.loop(0, model // chunk)
    def _(c):
        cut = head_cut(c, chunk)
        projected = jnp.dot(heads_ref[...], proj_ref[:, cut], preferred_element_type=jnp.float32)
        mixed = (residual_ref[:, cut].astype(jnp.float32) + projected).astype(jnp.bfloat16)
        mixed_ref[:, cut] = mixed
        mixed_wide = mixed.astype(jnp.float32)
        square_ref[...] += jnp.sum(mixed_wide * mixed_wide, axis=-1, keepdims=True)

    factor = lax.rsqrt(square_ref[...] * (1.0 / model) + 1e-06)

    @pl.loop(0, model // chunk)
    def _(c):
        cut = head_cut(c, chunk)
        mixed_wide = mixed_ref[:, cut].astype(jnp.float32)
        normed_ref[:, cut] = (mixed_wide * factor * gain_ref[:, cut]).astype(jnp.bfloat16)

    for which in range(4):
        for j in range(1, per):
            scatter(j, which).wait_send()
    for which in range(3):
        for q in range(per):
            for step in (1, -1):

                @pl.when(hops(step, q))
                def _():
                    hop(step, q, which, False).wait_send()

    for it in range(last):
        give(it).wait_send()


def attend(count, query_rows, key_rows, value_rows, ids, mix_lambda, residual, gain, out_weight):
    length, width = query_rows.shape
    per = REACH + 1
    wide, value_dim = width // per, value_rows.shape[1] // per
    rows, model = residual.shape
    blocks = 3 * REACH + 1
    outs = length // rows * per
    kept = jnp.bfloat16
    shape = jax.ShapeDtypeStruct((rows, model), kept)
    dma = pltpu.SemaphoreType.DMA
    smem = pl.BlockSpec(memory_space=pltpu.SMEM)
    anywhere = pl.BlockSpec(memory_space=pl.ANY)
    return pl.pallas_call(
        functools.partial(attend_kernel, count // per),
        out_shape=[shape, shape],
        in_specs=[smem] + [VMEM] * 6 + [anywhere],
        out_specs=[VMEM] * 2,
        scratch_shapes=[
            pltpu.VMEM((per, length, wide), kept),
            pltpu.VMEM((blocks, length, wide), kept),
            pltpu.VMEM((blocks, length, value_dim), kept),
            pltpu.VMEM((1, blocks * length), jnp.int32),
            pltpu.VMEM((outs, rows, value_dim), kept),
            pltpu.VMEM((rows, outs * value_dim), kept),
            pltpu.VMEM(out_weight.shape, kept),
            pltpu.VMEM((rows, 1), jnp.float32),
            dma,
            dma((per - 1, 4)),
            dma((per - 1, 4)),
            dma((2, per, 3)),
            dma((2, per, 3)),
            dma((outs,)),
            dma((outs,)),
        ],
        compiler_params=pltpu.CompilerParams(collective_id=0, has_side_effects=True),
        name="attend",
    )(mix_lambda, query_rows, key_rows, value_rows, ids, residual, gain, out_weight)


def greet_all(count, me, core):
    barrier = pltpu.get_barrier_semaphore()
    pl.semaphore_signal(barrier, inc=1, device_id=(me, 1 - core), device_id_type=MESH)

    @pl.loop(1, count)
    def _(step):
        pl.semaphore_signal(
            barrier, inc=1, device_id=((me + step) % count, core), device_id_type=MESH
        )

    pl.semaphore_wait(barrier, count)


def experts_kernel(
    count,
    normed_ref,
    slot_ref,
    gate_hbm,
    up_hbm,
    down_hbm,
    back_ref,
    dense_ref,
    slots_ref,
    rows_ref,
    pack_ref,
    part_ref,
    far_ref,
    sum_ref,
    hidden_ref,
    gate_ref,
    up_ref,
    down_ref,
    load_sem,
    slot_send,
    slot_recv,
    line_send,
    line_recv,
    flat_send,
    flat_recv,
    pass_sem,
    come_sem,
    swap_sem,
    half_sem,
    give_sem,
    take_sem,
):
    me, core = lax.axis_index("sp"), lax.axis_index("tp")
    per, capacity, model = rows_ref.shape[2:]
    groups = count // per
    tokens = dense_ref.shape[1]
    pieces = line_recv.shape[1]
    piece = tokens // pieces
    g, p = me // per, me % per
    greet_all(count, me, core)

    def remote(source, target, sent, came, at, side):
        return pltpu.make_async_remote_copy(
            src_ref=source,
            dst_ref=target,
            send_sem=sent,
            recv_sem=came,
            device_id=(at, side),
            device_id_type=MESH,
        )

    def tell(t, source):
        to = (g + t) % groups
        return remote(
            slot_ref, slots_ref.at[source], slot_send.at[t], slot_recv.at[t], to * per + p, core
        )

    def inside(s):
        return jnp.logical_and(s >= 0, s < groups)

    def line(step, s, part, own):
        cut = pl.ds(part * piece, piece)
        return remote(
            normed_ref.at[cut] if own else dense_ref.at[s, cut],
            dense_ref.at[s, cut],
            line_send.at[(1 - step) // 2, s, part],
            line_recv.at[s, part],
            me + step * per,
            core,
        )

    def flat(s, j):
        to = (p + j) % per
        return remote(
            pack_ref.at[s, to],
            rows_ref.at[s, core, p],
            flat_send.at[s, j],
            flat_recv.at[s, j],
            g * per + to,
            core,
        )

    def flat_came(s, j):
        source = (p + per - j) % per
        return remote(
            pack_ref.at[s, source],
            rows_ref.at[s, core, source],
            flat_send.at[s, j],
            flat_recv.at[s, j],
            g * per + source,
            core,
        )

    def forward(s, q, side):
        block = rows_ref.at[s, side, q]
        return remote(block, block, pass_sem.at[s, q], come_sem.at[s, q], me, 1 - core)

    def swap(s):
        return remote(
            part_ref.at[s, 1 - core], far_ref.at[s], swap_sem.at[s], half_sem.at[s], me, 1 - core
        )

    def home(s, q):
        return remote(
            sum_ref.at[s, q],
            back_ref.at[me],
            give_sem.at[s, q],
            take_sem.at[g, p],
            s * per + q,
            core,
        )

    def came_home(s, q):
        return remote(
            sum_ref.at[s, q],
            back_ref.at[s * per + q],
            give_sem.at[s, q],
            take_sem.at[s, q],
            s * per + q,
            core,
        )

    for t in range(1, groups):
        tell(t, g).start()
    for part in range(pieces):
        for step in (1, -1):

            @pl.when(inside(g + step))
            def _():
                line(step, g, part, True).start()

    loads = [
        pltpu.make_async_copy(source, target, load_sem.at[which])
        for which, (source, target) in enumerate(
            ((gate_hbm, gate_ref), (up_hbm, up_ref), (down_hbm, down_ref))
        )
    ]
    for load in loads:
        load.start()
    dense_ref[g] = normed_ref[...]
    slots_ref[g] = slot_ref[...]

    lead = 1 - 2 * (2 * g // groups)
    wide = min(256, model)

    def pack(s):
        slot = lax.broadcasted_iota(jnp.int32, (per * capacity, tokens), 0) + g * per * capacity
        table = slots_ref[s]
        chosen = jnp.logical_or(slot == table[:1], slot == table[1:2])
        spread = jnp.where(chosen, 1.0, 0.0).astype(dense_ref.dtype)

        @pl.loop(0, model // wide)
        def _(c):
            cut = pl.ds(pl.multiple_of(c * wide, wide), wide)
            taken = jnp.dot(spread, dense_ref[s, :, cut], preferred_element_type=jnp.float32)
            pack_ref[s, :, :, cut] = taken.astype(pack_ref.dtype).reshape(per, capacity, wide)

        rows_ref[s, core, p] = pack_ref[s, p]
        for j in range(1, per):
            flat(s, j).start()
        forward(s, p, core).start()

    def expert(s):
        for j in range(1, per):
            flat_came(s, j).wait_recv()
            forward(s, (p + per - j) % per, core).start()
        for q in range(per):
            forward(s, q, 1 - core).wait_recv()
        rows, width = hidden_ref.shape

        @pl.loop(0, width // wide)
        def _(c):
            cut = pl.ds(pl.multiple_of(c * wide, wide), wide)
            taken = rows_ref[s].reshape(rows, model)
            gate = jnp.dot(taken, gate_ref[:, cut], preferred_element_type=jnp.float32)
            upward = jnp.dot(taken, up_ref[:, cut], preferred_element_type=jnp.float32)
            hidden_ref[:, cut] = (gate / (1.0 + jnp.exp(-gate)) * upward).astype(hidden_ref.dtype)

        @pl.loop(0, model // wide)
        def _(c):
            cut = pl.ds(pl.multiple_of(c * wide, wide), wide)
            product = jnp.dot(
                hidden_ref[...], down_ref[:, cut], preferred_element_type=jnp.float32
            ).astype(part_ref.dtype)
            part_ref[s, :, :, :, cut] = product.reshape(part_ref.shape[1:4] + (wide,))

        swap(s).start()
        swap(s).wait_recv()

        def give(q):
            @pl.when(jnp.logical_or(s != g, q != p))
            def _():
                home(s, q).start()

        for q in range(per):
            mine = part_ref[s, core, q].astype(jnp.float32)
            sum_ref[s, q] = (mine + far_ref[s, q].astype(jnp.float32)).astype(sum_ref.dtype)
            if q > 0:
                give(q - 1)
        give(per - 1)

    @pl.loop(0, groups + 1)
    def _(d):
        @pl.when(d == 1)
        def _():
            for t in range(1, groups):
                tell(t, (g + groups - t) % groups).wait_recv()
            for load in loads:
                load.wait()

        def source_of(at, k):
            s = g + lead * (1 - 2 * k) * at
            return s, jnp.logical_and(inside(s), jnp.logical_or(at > 0, k == 0))

        for part in range(pieces):
            for k in range(2):
                s, valid = source_of(d, k)
                step = lead * (2 * k - 1)

                @pl.when(jnp.logical_and(valid, d > 0))
                def _():
                    line(step, s, part, False).wait_recv()

                    @pl.when(inside(g + step))
                    def _():
                        line(step, s, part, False).start()

        @pl.loop(0, 2)
        def _(k):
            s, valid = source_of(d, k)

            @pl.when(valid)
            def _():
                pack(s)

        @pl.loop(0, 2)
        def _(k):
            s, valid = source_of(d - 1, k)

            @pl.when(jnp.logical_and(valid, d > 0))
            def _():
                expert(s)

    back_ref[me] = sum_ref[g, p]

    @pl.loop(0, groups)
    def _(s):
        for q in range(per):

            @pl.when(jnp.logical_or(s != g, q != p))
            def _():
                came_home(s, q).wait_recv()
                home(s, q).wait_send()

            forward(s, q, core).wait_send()
        for j in range(1, per):
            flat(s, j).wait_send()
        swap(s).wait_send()
        for step in (1, -1):
            sent = s <= g if step > 0 else s >= g

            @pl.when(jnp.logical_and(sent, inside(g + step)))
            def _():
                for part in range(pieces):
                    line(step, s, part, False).wait_send()

    for t in range(1, groups):
        tell(t, g).wait_send()


def run_experts(count, capacity, normed, slots, gate_weight, up_weight, down_weight):
    tokens, model = normed.shape
    per = REACH + 1
    groups = count // per
    hidden = gate_weight.shape[1]
    kept = normed.dtype
    pieces = 2
    dma = pltpu.SemaphoreType.DMA
    each = dma((groups, per))
    whole = dma((groups,))
    anywhere = pl.BlockSpec(memory_space=pl.ANY)
    return pl.pallas_call(
        functools.partial(experts_kernel, count),
        out_shape=jax.ShapeDtypeStruct((count, capacity, model), kept),
        in_specs=[VMEM, VMEM, anywhere, anywhere, anywhere],
        out_specs=VMEM,
        scratch_shapes=[
            pltpu.VMEM((groups, tokens, model), kept),
            pltpu.VMEM((groups,) + slots.shape, jnp.int32),
            pltpu.VMEM((groups, 2, per, capacity, model), kept),
            pltpu.VMEM((groups, per, capacity, model), kept),
            pltpu.VMEM((groups, 2, per, capacity, model), kept),
            pltpu.VMEM((groups, per, capacity, model), kept),
            pltpu.VMEM((groups, per, capacity, model), kept),
            pltpu.VMEM((2 * per * capacity, hidden), kept),
            pltpu.VMEM(gate_weight.shape, kept),
            pltpu.VMEM(up_weight.shape, kept),
            pltpu.VMEM(down_weight.shape, kept),
            dma((3,)),
            whole,
            whole,
            dma((2, groups, pieces)),
            dma((groups, pieces)),
            each,
            each,
            each,
            each,
            whole,
            whole,
            each,
            each,
        ],
        compiler_params=pltpu.CompilerParams(collective_id=1, has_side_effects=True),
        name="experts",
    )(normed, slots, gate_weight, up_weight, down_weight)


def slots_of(routes, experts, capacity):
    flat_routes = routes.reshape(-1)
    table = (flat_routes[:, None] == jnp.arange(experts, dtype=jnp.int32)[None, :]).astype(
        jnp.float32
    )
    count = table.shape[0]
    before = jnp.tril(jnp.ones((count, count), jnp.bfloat16), -1)
    earlier = jnp.dot(before, table.astype(jnp.bfloat16), preferred_element_type=jnp.float32)
    rank = jnp.sum(earlier * table, axis=1).astype(jnp.int32)
    return (flat_routes * capacity + rank).reshape(routes.shape)


def on_device(
    residual,
    query_rows,
    key_rows,
    value_rows,
    mix_lambda,
    documents,
    out_weight,
    norm_gain,
    gate_weight,
    up_weight,
    down_weight,
    routes,
    route_weights,
):
    length = query_rows.shape[0]
    model_width = residual.shape[1]
    experts = lax.axis_size("sp")
    capacity = 2 * length // experts
    top_count = routes.shape[1]
    mixed, normed = attend(
        experts,
        query_rows,
        key_rows,
        value_rows,
        documents.reshape(1, length),
        mix_lambda,
        residual,
        norm_gain.reshape(1, model_width),
        out_weight,
    )
    mixed_wide = mixed.astype(jnp.float32)
    slots = slots_of(routes, experts, capacity)
    places = jnp.arange(experts * capacity, dtype=jnp.int32)
    returned = run_experts(
        experts, capacity, normed, slots.T, gate_weight[0], up_weight[0], down_weight[0]
    ).reshape(-1, model_width)
    weighted = 0.0
    for which in range(top_count):
        pick = (slots[:, which][:, None] == places[None, :]).astype(jnp.bfloat16)
        picked = jnp.dot(pick, returned, preferred_element_type=jnp.float32)
        weighted = weighted + picked * route_weights[:, which][:, None]
    return (mixed_wide + weighted).astype(jnp.bfloat16)


def solution(mesh):
    placed = (
        P(("sp", "tp"), None),
        P("sp", "tp"),
        P("sp", "tp"),
        P("sp", "tp"),
        P("tp"),
        P("sp"),
        P(),
        P(),
        P("sp", None, "tp"),
        P("sp", None, "tp"),
        P("sp", "tp", None),
        P(("sp", "tp"), None),
        P(("sp", "tp"), None),
    )
    return jax.shard_map(
        on_device, mesh=mesh, in_specs=placed, out_specs=P(("sp", "tp"), None), check_vma=False
    )
```

```python
import functools

import jax
import jax.numpy as jnp
from jax import lax
from jax.experimental import pallas as pl
from jax.experimental.pallas import tpu as pltpu
from jax.sharding import PartitionSpec as P

HD = 64
REACH = 3
MESH = pl.DeviceIdType.MESH
VMEM = pl.BlockSpec(memory_space=pltpu.VMEM)


def attend_kernel(
    groups,
    lambda_ref,
    q_ref,
    k_ref,
    v_ref,
    id_ref,
    residual_ref,
    gain_ref,
    proj_hbm,
    mixed_ref,
    normed_ref,
    q_all,
    k_all,
    v_all,
    id_all,
    out_buf,
    heads_ref,
    proj_ref,
    square_ref,
    proj_sem,
    in_send,
    in_recv,
    hop_send,
    hop_recv,
    out_send,
    out_recv,
):
    me, core = lax.axis_index("sp"), lax.axis_index("tp")
    per = REACH + 1
    g, p = me // per, me % per
    length, wide = q_all.shape[1:]
    value_dim = v_all.shape[2]
    rows = mixed_ref.shape[0]
    cores = length // rows
    span = 2 * REACH + 1
    barrier = pltpu.get_barrier_semaphore()

    for side in range(cores):
        for j in range(per):

            @pl.when(jnp.logical_or(side != core, j > 0))
            def _():
                at = g * per + (p + j) % per
                pl.semaphore_signal(barrier, inc=1, device_id=(at, side), device_id_type=MESH)

    def beyond(step):
        return jnp.logical_and(g + step >= 0, g + step < groups)

    for step in (1, -1):

        @pl.when(beyond(step))
        def _():
            at = me + step * per
            pl.semaphore_signal(barrier, inc=1, device_id=(at, core), device_id_type=MESH)

    others = cores * per - 1
    pl.semaphore_wait(barrier, others + jnp.minimum(g, 1) + jnp.minimum(groups - 1 - g, 1))

    def remote(source, target, sent, came, at, side):
        return pltpu.make_async_remote_copy(
            src_ref=source,
            dst_ref=target,
            send_sem=sent,
            recv_sem=came,
            device_id=(at, side),
            device_id_type=MESH,
        )

    def head_cut(head, width):
        return pl.ds(pl.multiple_of(head * width, width), width)

    def id_cut(slot):
        return pl.ds(pl.multiple_of(slot * length, length), length)

    def own_part(which, head):
        return (
            id_ref,
            k_ref.at[:, head_cut(head, wide)],
            v_ref.at[:, head_cut(head, value_dim)],
            q_ref.at[:, head_cut(head, wide)],
        )[which]

    def place_of(which, slot):
        return (
            id_all.at[:, id_cut(slot)],
            k_all.at[slot],
            v_all.at[slot],
            q_all.at[slot - REACH],
        )[which]

    def scatter(j, which):
        to = (p + j) % per
        return remote(
            own_part(which, to),
            place_of(which, REACH + p),
            in_send.at[j - 1, which],
            in_recv.at[j - 1, which],
            g * per + to,
            core,
        )

    def scattered(j, which):
        source = (p + per - j) % per
        return remote(
            own_part(which, source),
            place_of(which, REACH + source),
            in_send.at[j - 1, which],
            in_recv.at[j - 1, which],
            g * per + source,
            core,
        )

    def hop(step, q, which, own):
        at = 0 if step > 0 else 1
        source = own_part(which, p) if own else place_of(which, REACH + q)
        return remote(
            source,
            place_of(which, REACH + q - step * per),
            hop_send.at[at, q, which],
            hop_recv.at[at, q, which],
            me + step * per,
            core,
        )

    def hopped(step, q, which):
        at = 0 if step > 0 else 1
        return remote(
            own_part(which, p),
            place_of(which, REACH + q - step * per),
            hop_send.at[at, q, which],
            hop_recv.at[at, q, which],
            me - step * per,
            core,
        )

    def hops(step, q):
        return jnp.logical_and(beyond(step), q > 0 if step > 0 else q < REACH)

    for which in range(4):
        for j in range(1, per):
            scatter(j, which).start()
        if which < 3:
            for step in (1, -1):

                @pl.when(hops(step, p))
                def _():
                    hop(step, p, which, True).start()

    load = pltpu.make_async_copy(proj_hbm, proj_ref, proj_sem)
    load.start()
    k_all[REACH + p] = k_ref[:, head_cut(p, wide)]
    v_all[REACH + p] = v_ref[:, head_cut(p, value_dim)]
    q_all[p] = q_ref[:, head_cut(p, wide)]
    id_all[:, id_cut(REACH + p)] = id_ref[...]
    for step in (1, -1):

        @pl.when(jnp.logical_not(beyond(-step)))
        def _():
            for slot in range(REACH):
                at = slot if step > 0 else span + slot
                k_all[at] = jnp.zeros_like(k_all[at])
                v_all[at] = jnp.zeros_like(v_all[at])
                id_all[:, at * length : (at + 1) * length] = jnp.full(
                    (1, length), -1, id_all.dtype
                )

    for which in range(3):
        for j in range(1, per):
            scattered(j, which).wait_recv()
            q = (p + per - j) % per
            for step in (1, -1):

                @pl.when(hops(step, q))
                def _():
                    hop(step, q, which, False).start()

    for j in range(1, per):
        scattered(j, 3).wait_recv()
    for which in range(3):
        for q in range(per):
            for step in (1, -1):
                if 0 <= REACH + q - step * per < span + REACH:

                    @pl.when(beyond(-step))
                    def _():
                        hopped(step, q, which).wait_recv()

    scale = jnp.asarray(HD ** (-0.5), q_all.dtype)
    contract = (((1,), (1,)), ((), ()))
    head = core * per + p

    def give(it):
        i, half = (p + 1 + it // cores) % per, (core + 1 + it) % cores
        return remote(
            out_buf.at[it],
            heads_ref.at[:, head_cut(head, value_dim)],
            out_send.at[it],
            out_recv.at[head],
            g * per + i,
            half,
        )

    def taken(source):
        return remote(
            out_buf.at[0],
            heads_ref.at[:, head_cut(source, value_dim)],
            out_send.at[0],
            out_recv.at[source],
            g * per + source % per,
            source // per,
        )

    @pl.loop(0, cores * per)
    def _(it):
        i, half = (p + 1 + it // cores) % per, (core + 1 + it) % cores
        first_row = pl.multiple_of(half * rows, rows)
        query = q_all[i, pl.ds(first_row, rows), :]
        lane = lax.broadcasted_iota(jnp.int32, query.shape, 1)
        own = id_all[:, pl.ds(pl.multiple_of((REACH + i) * length + half * rows, rows), rows)]
        own = jnp.transpose(jnp.broadcast_to(own, (128, rows)))[:, :1]
        ids = id_all[:, pl.ds(pl.multiple_of(i * length, length), span * length)]
        same = own == ids
        keys = k_all[pl.ds(i, span)].reshape(span * length, wide)
        values = v_all[pl.ds(i, span)].reshape(span * length, value_dim)

        def lifted(keep):
            part = jnp.where(keep, query * scale, jnp.zeros_like(query))
            scores = lax.dot_general(part, keys, contract, preferred_element_type=jnp.float32)
            masked = jnp.where(same, scores, -1e30)
            powers = jnp.exp(masked - jnp.max(masked, axis=-1, keepdims=True))
            return powers, jnp.sum(powers, axis=-1, keepdims=True)

        first, first_sum = lifted(lane < HD)
        second, second_sum = lifted(lane >= HD)
        weights = first * (1.0 / first_sum) - second * (lambda_ref[p] / second_sum)
        head_out = jnp.dot(
            weights.astype(jnp.bfloat16), values, preferred_element_type=jnp.float32
        )
        scaled = head_out * lax.rsqrt(
            jnp.mean(head_out * head_out, axis=-1, keepdims=True) + 1e-06
        )
        out_buf[it] = scaled.astype(jnp.bfloat16)

        @pl.when(it > 0)
        def _():
            give(it - 1).start()

    last = cores * per - 1
    heads_ref[:, head_cut(head, value_dim)] = out_buf[last]
    load.wait()
    for source in range(cores * per):

        @pl.when(source != head)
        def _():
            taken(source).wait_recv()

    model = mixed_ref.shape[1]
    chunk = min(1024, model)
    square_ref[...] = jnp.zeros_like(square_ref)

    @pl.loop(0, model // chunk)
    def _(c):
        cut = head_cut(c, chunk)
        projected = jnp.dot(heads_ref[...], proj_ref[:, cut], preferred_element_type=jnp.float32)
        mixed = (residual_ref[:, cut].astype(jnp.float32) + projected).astype(jnp.bfloat16)
        mixed_ref[:, cut] = mixed
        mixed_wide = mixed.astype(jnp.float32)
        square_ref[...] += jnp.sum(mixed_wide * mixed_wide, axis=-1, keepdims=True)

    factor = lax.rsqrt(square_ref[...] * (1.0 / model) + 1e-06)

    @pl.loop(0, model // chunk)
    def _(c):
        cut = head_cut(c, chunk)
        mixed_wide = mixed_ref[:, cut].astype(jnp.float32)
        normed_ref[:, cut] = (mixed_wide * factor * gain_ref[:, cut]).astype(jnp.bfloat16)

    for which in range(4):
        for j in range(1, per):
            scatter(j, which).wait_send()
    for which in range(3):
        for q in range(per):
            for step in (1, -1):

                @pl.when(hops(step, q))
                def _():
                    hop(step, q, which, False).wait_send()

    for it in range(last):
        give(it).wait_send()


def attend(count, query_rows, key_rows, value_rows, ids, mix_lambda, residual, gain, out_weight):
    length, width = query_rows.shape
    per = REACH + 1
    wide, value_dim = width // per, value_rows.shape[1] // per
    rows, model = residual.shape
    blocks = 3 * REACH + 1
    outs = length // rows * per
    kept = jnp.bfloat16
    shape = jax.ShapeDtypeStruct((rows, model), kept)
    dma = pltpu.SemaphoreType.DMA
    smem = pl.BlockSpec(memory_space=pltpu.SMEM)
    anywhere = pl.BlockSpec(memory_space=pl.ANY)
    return pl.pallas_call(
        functools.partial(attend_kernel, count // per),
        out_shape=[shape, shape],
        in_specs=[smem] + [VMEM] * 6 + [anywhere],
        out_specs=[VMEM] * 2,
        scratch_shapes=[
            pltpu.VMEM((per, length, wide), kept),
            pltpu.VMEM((blocks, length, wide), kept),
            pltpu.VMEM((blocks, length, value_dim), kept),
            pltpu.VMEM((1, blocks * length), jnp.int32),
            pltpu.VMEM((outs, rows, value_dim), kept),
            pltpu.VMEM((rows, outs * value_dim), kept),
            pltpu.VMEM(out_weight.shape, kept),
            pltpu.VMEM((rows, 1), jnp.float32),
            dma,
            dma((per - 1, 4)),
            dma((per - 1, 4)),
            dma((2, per, 3)),
            dma((2, per, 3)),
            dma((outs,)),
            dma((outs,)),
        ],
        compiler_params=pltpu.CompilerParams(collective_id=0, has_side_effects=True),
        name="attend",
    )(mix_lambda, query_rows, key_rows, value_rows, ids, residual, gain, out_weight)


def greet_all(count, me, core):
    barrier = pltpu.get_barrier_semaphore()
    pl.semaphore_signal(barrier, inc=1, device_id=(me, 1 - core), device_id_type=MESH)

    @pl.loop(1, count)
    def _(step):
        pl.semaphore_signal(
            barrier, inc=1, device_id=((me + step) % count, core), device_id_type=MESH
        )

    pl.semaphore_wait(barrier, count)


def experts_kernel(
    count,
    normed_ref,
    mixed_ref,
    routes_ref,
    share_ref,
    gate_hbm,
    up_hbm,
    down_hbm,
    out_ref,
    back_ref,
    dense_ref,
    slot_ref,
    slots_ref,
    rows_ref,
    pack_ref,
    part_ref,
    far_ref,
    sum_ref,
    hidden_ref,
    gate_ref,
    up_ref,
    down_ref,
    load_sem,
    slot_send,
    slot_recv,
    line_send,
    line_recv,
    flat_send,
    flat_recv,
    pass_sem,
    come_sem,
    swap_sem,
    half_sem,
    give_sem,
    take_sem,
):
    me, core = lax.axis_index("sp"), lax.axis_index("tp")
    per, capacity, model = rows_ref.shape[2:]
    groups = count // per
    tokens = dense_ref.shape[1]
    pieces = line_recv.shape[1]
    halves = half_sem.shape[1]
    g, p = me // per, me % per
    loads = [
        pltpu.make_async_copy(source, target, load_sem.at[which])
        for which, (source, target) in enumerate(
            ((gate_hbm, gate_ref), (up_hbm, up_ref), (down_hbm, down_ref))
        )
    ]
    for load in loads:
        load.start()
    slot_ref[...] = slots_of(routes_ref[...], count, capacity)
    dense_ref[g] = normed_ref[...]
    slots_ref[g] = slot_ref[...]
    greet_all(count, me, core)

    def remote(source, target, sent, came, at, side):
        return pltpu.make_async_remote_copy(
            src_ref=source,
            dst_ref=target,
            send_sem=sent,
            recv_sem=came,
            device_id=(at, side),
            device_id_type=MESH,
        )

    def tell(t, source):
        to = (g + t) % groups
        return remote(
            slot_ref, slots_ref.at[source], slot_send.at[t], slot_recv.at[t], to * per + p, core
        )

    def inside(s):
        return jnp.logical_and(s >= 0, s < groups)

    def part_cut(part, parts):
        width = model // parts
        return pl.ds(part * width, width)

    def line(step, s, part, own):
        cut = part_cut(part, pieces)
        return remote(
            normed_ref.at[:, cut] if own else dense_ref.at[s, :, cut],
            dense_ref.at[s, :, cut],
            line_send.at[(1 - step) // 2, s, part],
            line_recv.at[s, part],
            me + step * per,
            core,
        )

    def flat(s, j, part):
        to = (p + j) % per
        cut = part_cut(part, pieces)
        return remote(
            pack_ref.at[s, to, :, cut],
            rows_ref.at[s, core, p, :, cut],
            flat_send.at[s, j, part],
            flat_recv.at[s, j, part],
            g * per + to,
            core,
        )

    def flat_came(s, j, part):
        source = (p + per - j) % per
        cut = part_cut(part, pieces)
        return remote(
            pack_ref.at[s, source, :, cut],
            rows_ref.at[s, core, source, :, cut],
            flat_send.at[s, j, part],
            flat_recv.at[s, j, part],
            g * per + source,
            core,
        )

    def forward(s, q, side):
        block = rows_ref.at[s, side, q]
        return remote(block, block, pass_sem.at[s, q], come_sem.at[s, q], me, 1 - core)

    def swap(s, h):
        cut = part_cut(h, halves)
        return remote(
            part_ref.at[s, 1 - core, :, :, cut],
            far_ref.at[s, :, :, cut],
            swap_sem.at[s, h],
            half_sem.at[s, h],
            me,
            1 - core,
        )

    def home(s, q, h):
        cut = part_cut(h, halves)
        return remote(
            sum_ref.at[s, q, :, cut],
            back_ref.at[me, :, cut],
            give_sem.at[s, q, h],
            take_sem.at[g, p, h],
            s * per + q,
            core,
        )

    def came_home(s, q, h):
        cut = part_cut(h, halves)
        return remote(
            sum_ref.at[s, q, :, cut],
            back_ref.at[s * per + q, :, cut],
            give_sem.at[s, q, h],
            take_sem.at[s, q, h],
            s * per + q,
            core,
        )

    for t in range(1, groups):
        tell(t, g).start()
    for part in range(pieces):
        for step in (1, -1):

            @pl.when(inside(g + step))
            def _():
                line(step, g, part, True).start()

    lead = 1 - 2 * (2 * g // groups)
    wide = min(1024, model)

    def pack(s, part):
        slot = lax.broadcasted_iota(jnp.int32, (per * capacity, tokens), 0) + g * per * capacity
        table = slots_ref[s]
        chosen = jnp.logical_or(slot == table[:1], slot == table[1:2])
        spread = jnp.where(chosen, 1.0, 0.0).astype(dense_ref.dtype)
        cut = part_cut(part, pieces)
        taken = jnp.dot(spread, dense_ref[s, :, cut], preferred_element_type=jnp.float32)
        pack_ref[s, :, :, cut] = taken.astype(pack_ref.dtype).reshape(per, capacity, -1)
        rows_ref[s, core, p, :, cut] = pack_ref[s, p, :, cut]
        for j in range(1, per):
            flat(s, j, part).start()
        if part == pieces - 1:
            forward(s, p, core).start()

    def expert(s):
        for j in range(1, per):
            for part in range(pieces):
                flat_came(s, j, part).wait_recv()
            forward(s, (p + per - j) % per, core).start()
        for q in range(per):
            forward(s, q, 1 - core).wait_recv()
        rows, width = hidden_ref.shape

        @pl.loop(0, width // wide)
        def _(c):
            cut = pl.ds(pl.multiple_of(c * wide, wide), wide)
            taken = rows_ref[s].reshape(rows, model)
            gate = jnp.dot(taken, gate_ref[:, cut], preferred_element_type=jnp.float32)
            upward = jnp.dot(taken, up_ref[:, cut], preferred_element_type=jnp.float32)
            hidden_ref[:, cut] = (gate / (1.0 + jnp.exp(-gate)) * upward).astype(hidden_ref.dtype)

        for h in range(halves):
            width = model // halves

            @pl.loop(0, width // wide)
            def _(c):
                cut = pl.ds(pl.multiple_of(h * width + c * wide, wide), wide)
                product = jnp.dot(
                    hidden_ref[...], down_ref[:, cut], preferred_element_type=jnp.float32
                ).astype(part_ref.dtype)
                part_ref[s, :, :, :, cut] = product.reshape(part_ref.shape[1:4] + (wide,))

            swap(s, h).start()

        def give(q, h):
            @pl.when(jnp.logical_or(s != g, q != p))
            def _():
                home(s, q, h).start()

        for h in range(halves):
            swap(s, h).wait_recv()
            cut = part_cut(h, halves)
            for q in range(per):
                mine = part_ref[s, core, q, :, cut].astype(jnp.float32)
                sum_ref[s, q, :, cut] = (mine + far_ref[s, q, :, cut].astype(jnp.float32)).astype(
                    sum_ref.dtype
                )
                if q > 0:
                    give(q - 1, h)
            give(per - 1, h)

    for part in range(pieces):
        pack(g, part)
    for t in range(1, groups):
        tell(t, (g + groups - t) % groups).wait_recv()
    for load in loads:
        load.wait()

    @pl.loop(1, groups + 1)
    def _(d):
        for part in range(pieces):
            for k in range(2):
                s = g + lead * (1 - 2 * k) * d
                step = lead * (2 * k - 1)

                @pl.when(inside(s))
                def _():
                    line(step, s, part, False).wait_recv()

                    @pl.when(inside(g + step))
                    def _():
                        line(step, s, part, False).start()

            @pl.loop(0, 2)
            def _(k):
                s = g + lead * (1 - 2 * k) * d

                @pl.when(inside(s))
                def _():
                    pack(s, part)

        @pl.loop(0, 2)
        def _(k):
            s = g - lead * (d - 1) + k * lead * (2 * d - 1)

            @pl.when(inside(s))
            def _():
                expert(s)

    back_ref[me] = sum_ref[g, p]

    @pl.loop(0, groups)
    def _(s):
        for q in range(per):

            @pl.when(jnp.logical_or(s != g, q != p))
            def _():
                for h in range(halves):
                    came_home(s, q, h).wait_recv()

    places = lax.broadcasted_iota(jnp.int32, (tokens, count * capacity), 1)

    def upright(row):
        return jnp.transpose(jnp.broadcast_to(row, (128, tokens)))[:, :1]

    picks = []
    for k in range(routes_ref.shape[0]):
        chosen = upright(slot_ref[k : k + 1, :]) == places
        picks.append(
            (jnp.where(chosen, 1.0, 0.0).astype(back_ref.dtype), upright(share_ref[k : k + 1, :]))
        )

    @pl.loop(0, model // wide)
    def _(c):
        cut = pl.ds(pl.multiple_of(c * wide, wide), wide)
        returned = back_ref[:, :, cut].reshape(count * capacity, wide)
        weighted = 0.0
        for pick, share in picks:
            weighted += jnp.dot(pick, returned, preferred_element_type=jnp.float32) * share
        out_ref[:, cut] = (mixed_ref[:, cut].astype(jnp.float32) + weighted).astype(out_ref.dtype)

    @pl.loop(0, groups)
    def _(s):
        for q in range(per):

            @pl.when(jnp.logical_or(s != g, q != p))
            def _():
                for h in range(halves):
                    home(s, q, h).wait_send()

            forward(s, q, core).wait_send()
        for j in range(1, per):
            for part in range(pieces):
                flat(s, j, part).wait_send()
        for h in range(halves):
            swap(s, h).wait_send()
        for step in (1, -1):
            sent = s <= g if step > 0 else s >= g

            @pl.when(jnp.logical_and(sent, inside(g + step)))
            def _():
                for part in range(pieces):
                    line(step, s, part, False).wait_send()

    for t in range(1, groups):
        tell(t, g).wait_send()


def run_experts(count, capacity, normed, mixed, routes, shares, gate_weight, up_weight, down_weight):
    tokens, model = normed.shape
    per = REACH + 1
    groups = count // per
    hidden = gate_weight.shape[1]
    kept = normed.dtype
    pieces, halves = 1, 2
    dma = pltpu.SemaphoreType.DMA
    each = dma((groups, per))
    whole = dma((groups,))
    anywhere = pl.BlockSpec(memory_space=pl.ANY)
    return pl.pallas_call(
        functools.partial(experts_kernel, count),
        out_shape=jax.ShapeDtypeStruct((tokens, model), kept),
        in_specs=[VMEM] * 4 + [anywhere] * 3,
        out_specs=VMEM,
        scratch_shapes=[
            pltpu.VMEM((count, capacity, model), kept),
            pltpu.VMEM((groups, tokens, model), kept),
            pltpu.VMEM(routes.shape, jnp.int32),
            pltpu.VMEM((groups,) + routes.shape, jnp.int32),
            pltpu.VMEM((groups, 2, per, capacity, model), kept),
            pltpu.VMEM((groups, per, capacity, model), kept),
            pltpu.VMEM((groups, 2, per, capacity, model), kept),
            pltpu.VMEM((groups, per, capacity, model), kept),
            pltpu.VMEM((groups, per, capacity, model), kept),
            pltpu.VMEM((2 * per * capacity, hidden), kept),
            pltpu.VMEM(gate_weight.shape, kept),
            pltpu.VMEM(up_weight.shape, kept),
            pltpu.VMEM(down_weight.shape, kept),
            dma((3,)),
            whole,
            whole,
            dma((2, groups, pieces)),
            dma((groups, pieces)),
            dma((groups, per, pieces)),
            dma((groups, per, pieces)),
            each,
            each,
            dma((groups, halves)),
            dma((groups, halves)),
            dma((groups, per, halves)),
            dma((groups, per, halves)),
        ],
        compiler_params=pltpu.CompilerParams(collective_id=1, has_side_effects=True),
        name="experts",
    )(normed, mixed, routes, shares, gate_weight, up_weight, down_weight)


def slots_of(routes, experts, capacity):
    tokens = routes.shape[1]
    expert = lax.broadcasted_iota(jnp.int32, (experts, tokens), 0)
    earlier = lax.broadcasted_iota(jnp.int32, (tokens, tokens), 0)
    later = lax.broadcasted_iota(jnp.int32, (tokens, tokens), 1)
    before = jnp.where(earlier < later, 1.0, 0.0).astype(jnp.bfloat16)
    taken, slots = 0.0, []
    for k in range(routes.shape[0]):
        named = jnp.where(expert == routes[k : k + 1], 1.0, 0.0)
        ahead = jnp.dot(named.astype(jnp.bfloat16), before, preferred_element_type=jnp.float32)
        rank = jnp.sum(named * (ahead + taken), axis=0, keepdims=True)
        taken = taken + jnp.sum(named, axis=1, keepdims=True)
        slots.append(routes[k : k + 1] * capacity + rank.astype(jnp.int32))
    return jnp.concatenate(slots, axis=0)


def on_device(
    residual,
    query_rows,
    key_rows,
    value_rows,
    mix_lambda,
    documents,
    out_weight,
    norm_gain,
    gate_weight,
    up_weight,
    down_weight,
    routes,
    route_weights,
):
    length = query_rows.shape[0]
    model_width = residual.shape[1]
    experts = lax.axis_size("sp")
    capacity = 2 * length // experts
    mixed, normed = attend(
        experts,
        query_rows,
        key_rows,
        value_rows,
        documents.reshape(1, length),
        mix_lambda,
        residual,
        norm_gain.reshape(1, model_width),
        out_weight,
    )
    return run_experts(
        experts,
        capacity,
        normed,
        mixed,
        routes.T,
        route_weights.T,
        gate_weight[0],
        up_weight[0],
        down_weight[0],
    )


def solution(mesh):
    placed = (
        P(("sp", "tp"), None),
        P("sp", "tp"),
        P("sp", "tp"),
        P("sp", "tp"),
        P("tp"),
        P("sp"),
        P(),
        P(),
        P("sp", None, "tp"),
        P("sp", None, "tp"),
        P("sp", "tp", None),
        P(("sp", "tp"), None),
        P(("sp", "tp"), None),
    )
    return jax.shard_map(
        on_device, mesh=mesh, in_specs=placed, out_specs=P(("sp", "tp"), None), check_vma=False
    )
```
